32 devices in a mesh: kv: 8 (over z, y), tp: 4 (over x, core).
Axes of the slice: x: 2, y: 2, z: 4, core: 2. Of those that a mesh axis runs over, the one named last changes fastest.
Arguments:
- activations: bfloat16 [64, 4096], P(None, ('kv', 'tp')), may hold values from -60 to 60
- mixer_gain: bfloat16 [4096], P(('kv', 'tp')), may hold values from 0.099609375 to 1.8984375
- channel_gain: bfloat16 [4096], P(('kv', 'tp')), may hold values from 0.099609375 to 1.8984375
- query_weight: bfloat16 [4096, 4096], P('kv', 'tp'), may hold values from -0.09375 to 0.09375
- key_weight: bfloat16 [4096, 4096], P('kv', 'tp'), may hold values from -0.09375 to 0.09375
- value_weight: bfloat16 [4096, 8192], P('kv', 'tp'), may hold values from -0.09375 to 0.09375
- gate_weight: bfloat16 [4096, 8192], P('kv', 'tp'), may hold values from -0.09375 to 0.09375
- output_weight: bfloat16 [8192, 4096], P('tp', 'kv'), may hold values from -0.1875 to 0.1875
- up_weight: bfloat16 [4096, 16384], P('kv', 'tp'), may hold values from -0.09375 to 0.09375
- down_weight: bfloat16 [16384, 4096], P('tp', 'kv'), may hold values from -0.046875 to 0.046875
- state_in: float32 [64, 16, 256, 512], P('kv', 'tp'), may hold values from -0.5 to 0.5
Outputs:
- activations_out: bfloat16 [64, 4096], P(None, ('kv', 'tp'))
- state_out: float32 [64, 16, 256, 512], P('kv', 'tp')
The draws below stay inside these ranges and needn't reach their ends.
All inputs are finite; a program needn't handle non-finite values.
Results may differ from the reference program's by a relative error of at most 0.022.
Values may be sent and summed in bfloat16 or wider, within the bound.
A program may use at most 128 MiB of HBM per device.

```python
import jax
import jax.numpy as jnp
from jax import lax

D = 4096
HEADS = 16
DK = 256
DV = 512
FF = 16384
BATCH = 64
QK = 4096
RV = 8192
N_TP = 4


def draw_activations(key, part):
    base_key, row_key = jax.random.split(key, 2)
    columns = jnp.exp(jnp.linspace(0.0, jnp.log(3.0), D, dtype=jnp.float32))
    base = jnp.clip(jax.random.normal(base_key, (BATCH, D), jnp.float32), -5.0, 5.0)
    scales = jnp.exp(jax.random.uniform(row_key, (BATCH, 1), jnp.float32, jnp.log(0.3), jnp.log(3.0)))
    return jnp.clip(base * scales * columns, -60.0, 60.0).astype(jnp.bfloat16)


def level_of(key, extent, shards, least, high):
    factor_of, own = 1.0, jax.random.fold_in(key, 6)
    for axis_at, shards_of in shards:
        heights = jnp.exp(jax.random.uniform(jax.random.fold_in(own, axis_at), (shards_of,), jnp.float32, least / len(shards), high / len(shards)))
        factor_of = factor_of * jnp.repeat(heights, extent[axis_at] // shards_of).reshape([-1 if axis == axis_at else 1 for axis in range(len(extent))])
    return factor_of


def normal_values(own_key, dims, spread, most, pieces=(), kind=jnp.bfloat16):
    values = spread * jax.random.normal(own_key, dims, jnp.float32)
    if pieces:
        values = values * level_of(own_key, dims, pieces, -0.22, 0.18)
    return jnp.clip(values, -most, most).astype(kind)


def setup_inputs(seed: int = 0) -> dict:
    key_list = jax.random.split(jax.random.key(seed), 12)
    activations = draw_activations(jax.random.fold_in(key_list[11], 71), 0)
    mixer_gain = jnp.clip(1.0 + 0.18 * jax.random.normal(key_list[1], (D,), jnp.float32), 0.099609375, 1.8984375).astype(jnp.bfloat16)
    channel_gain = jnp.clip(1.0 + 0.18 * jax.random.normal(key_list[2], (D,), jnp.float32), 0.099609375, 1.8984375).astype(jnp.bfloat16)
    query_weight = normal_values(key_list[3], (D, QK), D ** -0.5, 0.09375, ((0, 8), (1, 4)))
    key_weight = normal_values(key_list[4], (D, QK), D ** -0.5, 0.09375, ((0, 8), (1, 4)))
    value_weight = normal_values(key_list[5], (D, RV), D ** -0.5, 0.09375, ((0, 8), (1, 4)))
    gate_weight = normal_values(key_list[6], (D, RV), D ** -0.5, 0.09375, ((0, 8), (1, 4)))
    output_weight = normal_values(key_list[7], (RV, D), (RV // 8) ** -0.5, 0.1875, ((0, 4), (1, 8)))
    up_weight = normal_values(key_list[8], (D, FF), D ** -0.5, 0.09375, ((0, 8), (1, 4)))
    down_weight = normal_values(key_list[9], (FF, D), FF ** -0.5, 0.046875, ((0, 4), (1, 8)))
    state_in = normal_values(key_list[10], (BATCH, HEADS, DK, DV), 0.06, 0.5, ((0, 8), (1, 4)), jnp.float32)
    return dict(activations=activations, mixer_gain=mixer_gain, channel_gain=channel_gain, query_weight=query_weight, key_weight=key_weight, value_weight=value_weight, gate_weight=gate_weight, output_weight=output_weight, up_weight=up_weight, down_weight=down_weight, state_in=state_in)


EPS = 1e-06

def head_decays(count):
    index = jnp.arange(count, dtype=jnp.float32)
    return 1.0 - 2.0 ** (-1.0 - 6.0 * index / (count - 1))

def summed_blocks(left, right, parts):
    width = left.shape[1] // parts
    total = jnp.zeros((left.shape[0], right.shape[1]), jnp.float32)
    for index in range(parts):
        term = jnp.dot(left[:, index * width:(index + 1) * width], right[index * width:(index + 1) * width], preferred_element_type=jnp.float32)
        total = total + lax.optimization_barrier(term.astype(jnp.bfloat16)).astype(jnp.float32)
    return total

def reference(activations, mixer_gain, channel_gain, query_weight, key_weight, value_weight, gate_weight, output_weight, up_weight, down_weight, state_in):
    stream = activations.astype(jnp.float32)
    scale_rows = lax.rsqrt(lax.optimization_barrier(jnp.sum(stream * stream, axis=1, keepdims=True)) / D + EPS)
    normed = (stream * mixer_gain.astype(jnp.float32)).astype(jnp.bfloat16)
    query = scale_rows * jnp.dot(normed, query_weight, preferred_element_type=jnp.float32)
    key = scale_rows * jnp.dot(normed, key_weight, preferred_element_type=jnp.float32) * DK ** (-0.5)
    value = scale_rows * jnp.dot(normed, value_weight, preferred_element_type=jnp.float32)
    gate = scale_rows * jnp.dot(normed, gate_weight, preferred_element_type=jnp.float32)
    rates = head_decays(HEADS)

    def advance(inputs):
        query_row, key_row, value_row, old_state = inputs
        query_heads = query_row.reshape(HEADS, DK)
        key_heads = key_row.reshape(HEADS, DK)
        value_heads = value_row.reshape(HEADS, DV)
        new_state = rates[:, None, None] * old_state + key_heads[:, :, None] * value_heads[:, None, :]
        output = jnp.einsum('hd,hde->he', query_heads, new_state, precision=lax.Precision.HIGHEST)
        return (new_state, output)
    state_out, retained = lax.map(advance, (query, key, value, state_in))
    retained = retained * lax.rsqrt(lax.optimization_barrier(jnp.mean(retained * retained, axis=2, keepdims=True)) + EPS)
    mixed = (jax.nn.silu(gate) * retained.reshape(retained.shape[0], HEADS * DV)).astype(jnp.bfloat16)
    attention = summed_blocks(mixed, output_weight, N_TP)
    middle = (stream + attention).astype(jnp.bfloat16)
    middle = lax.optimization_barrier(middle).astype(jnp.float32)
    channel_scale = lax.rsqrt(lax.optimization_barrier(jnp.sum(middle * middle, axis=1, keepdims=True)) / D + EPS)
    channel_normed = (middle * channel_gain.astype(jnp.float32)).astype(jnp.bfloat16)
    lifted = channel_scale * jnp.dot(channel_normed, up_weight, preferred_element_type=jnp.float32)
    hidden = jnp.square(jax.nn.relu(lifted)).astype(jnp.bfloat16)
    lowered = summed_blocks(hidden, down_weight, N_TP)
    return ((middle + lowered).astype(jnp.bfloat16), state_out)
```

```python
import functools

import jax
import jax.numpy as jnp
from jax import lax
from jax.experimental import pallas as pl
from jax.experimental.pallas import tpu as pltpu
from jax.sharding import PartitionSpec as P

HEADS = 16
EPS = 1e-06
MESH = pl.DeviceIdType.MESH
F32 = jnp.float32
BF16 = jnp.bfloat16
DMA = pltpu.SemaphoreType.DMA
PAIR = 2
LAG = 2


def head_decays(count):
    index = jnp.arange(count, dtype=jnp.float32)
    return 1.0 - 2.0 ** (-1.0 - 6.0 * index / (count - 1))


def put(src, dst, send_sem, recv_sem, where):
    copy = pltpu.make_async_remote_copy(
        src_ref=src,
        dst_ref=dst,
        send_sem=send_sem,
        recv_sem=recv_sem,
        device_id=where,
        device_id_type=MESH,
    )
    copy.start()
    return copy


def greet(kv, tp, n_kv, n_tp):
    barrier = pltpu.get_barrier_semaphore()
    for d in range(1, n_tp):
        pl.semaphore_signal(
            barrier, inc=1, device_id={"tp": lax.rem(tp + d, n_tp)}, device_id_type=MESH
        )
    for d in range(1, n_kv):
        pl.semaphore_signal(
            barrier, inc=1, device_id={"kv": lax.rem(kv + d, n_kv)}, device_id_type=MESH
        )
    pl.semaphore_wait(barrier, n_tp + n_kv - 2)


def tp_gather(buf, tp, n_tp, sems):
    return [
        put(
            buf.at[tp],
            buf.at[tp],
            sems.at[0, d - 1],
            sems.at[1, d - 1],
            {"tp": lax.rem(tp + d, n_tp)},
        )
        for d in range(1, n_tp)
    ]


def tp_scatter(src, dst, tp, n_tp, sems):
    copies = []
    for d in range(1, n_tp):
        peer = lax.rem(tp + d, n_tp)
        copies.append(
            put(src.at[peer], dst.at[d - 1], sems.at[0, d - 1], sems.at[1, d - 1], {"tp": peer})
        )
    return copies


def kv_scatter_small(src, dst, kv, n_kv, sems):
    copies = []
    for d in range(1, n_kv):
        peer = lax.rem(kv + d, n_kv)
        copies.append(
            put(src.at[peer], dst.at[d - 1], sems.at[0, d - 1], sems.at[1, d - 1], {"kv": peer})
        )
    return copies


def own_square_total(squares, sq_src, sq_dst, kv, n_kv, rows, sems):
    for g in range(n_kv):
        sq_src[g] = jnp.broadcast_to(squares[g * rows : (g + 1) * rows], sq_src.shape[1:])
    copies = kv_scatter_small(sq_src, sq_dst, kv, n_kv, sems)

    def finish():
        total = sq_src[kv]
        for d, copy in enumerate(copies):
            copy.wait_recv()
            total = total + sq_dst[d]
        return total[:, :1]

    return copies, finish


class PairScatter:
    def __init__(self, kv, n_kv, rows, part, got, summed, got2, sem_a, sem_b):
        self.n_z = n_kv // PAIR
        self.z, self.y = lax.div(kv, PAIR), lax.rem(kv, PAIR)
        self.rows = rows
        self.part, self.got, self.summed, self.got2 = part, got, summed, got2
        self.sem_a, self.sem_b = sem_a, sem_b
        self.first, self.second = {}, {}

    def start(self, p, value):
        rows = self.rows
        for z in range(self.n_z):
            for y in range(PAIR):
                at = (z * PAIR + y) * rows
                self.part[p, y, z] = value[at : at + rows].astype(BF16)
        other = 1 - self.y
        self.first[p] = put(
            self.part.at[p, other],
            self.got.at[p],
            self.sem_a.at[0, p],
            self.sem_a.at[1, p],
            {"kv": self.z * PAIR + other},
        )

    def middle(self, p):
        self.first[p].wait_recv()
        self.summed[p] = (self.part[p, self.y].astype(F32) + self.got[p].astype(F32)).astype(BF16)
        copies = []
        for d in range(1, self.n_z):
            peer = lax.rem(self.z + d, self.n_z)
            copies.append(
                put(
                    self.summed.at[p, peer],
                    self.got2.at[p, d - 1],
                    self.sem_b.at[0, p, d - 1],
                    self.sem_b.at[1, p, d - 1],
                    {"kv": peer * PAIR + self.y},
                )
            )
        self.second[p] = copies

    def finish(self, p):
        total = self.summed[p, self.z].astype(F32)
        for d, copy in enumerate(self.second[p]):
            copy.wait_recv()
            total = total + self.got2[p, d].astype(F32)
        return total

    def drain(self):
        for p in self.first:
            self.first[p].wait_send()
            for copy in self.second[p]:
                copy.wait_send()


class PairGather:
    def __init__(self, kv, n_kv, buf, sem_z, sem_y):
        self.n_z = n_kv // PAIR
        self.z, self.y = lax.div(kv, PAIR), lax.rem(kv, PAIR)
        self.buf, self.sem_z, self.sem_y = buf, sem_z, sem_y
        self.along, self.across = {}, {}

    def forward(self, p, d):
        z = lax.rem(self.z - d + self.n_z, self.n_z)
        self.across[p].append(
            put(
                self.buf.at[p, z, self.y],
                self.buf.at[p, z, self.y],
                self.sem_y.at[0, p, d],
                self.sem_y.at[1, p, d],
                {"kv": self.z * PAIR + 1 - self.y},
            )
        )

    def start(self, p):
        own = self.buf.at[p, self.z, self.y]
        self.along[p], self.across[p] = [], []
        for d in range(1, self.n_z):
            peer = lax.rem(self.z + d, self.n_z)
            self.along[p].append(
                put(
                    own,
                    own,
                    self.sem_z.at[0, p, d - 1],
                    self.sem_z.at[1, p, d - 1],
                    {"kv": peer * PAIR + self.y},
                )
            )
        self.forward(p, 0)

    def relay(self, p):
        for d, copy in enumerate(self.along[p]):
            copy.wait_recv()
            self.forward(p, d + 1)

    def finish(self, p):
        for copy in self.across[p]:
            copy.wait_recv()
        blocks = [
            self.buf[p, z, y].astype(F32) for z in range(self.n_z) for y in range(PAIR)
        ]
        return jnp.concatenate(blocks, axis=0).astype(BF16)

    def drain(self):
        for p in self.along:
            for copy in self.along[p] + self.across[p]:
                copy.wait_send()


def project_kernel(
    sizes,
    x_ref,
    gain_ref,
    *refs,
):
    n_kv, n_tp, rows, width, counts, dim = sizes
    weights, refs = refs[:4], refs[4:]
    outs, refs = refs[:4], refs[4:]
    (xs, gains, w, part, got, summed, got2, sq_src, sq_dst) = refs[:9]
    (w_sem, x_sem, g_sem, sq_sem, sem_a, sem_b) = refs[9:]
    kv, tp = lax.axis_index("kv"), lax.axis_index("tp")
    pieces = [(i, j) for i, count in enumerate(counts) for j in range(count)]
    loads = []
    for p, (i, j) in enumerate(pieces):
        load = pltpu.make_async_copy(
            weights[i].at[:, pl.ds(j * width, width)], w.at[p], w_sem.at[p]
        )
        load.start()
        loads.append(load)
    xs[tp] = x_ref[...]
    gains[tp] = jnp.broadcast_to(gain_ref[...].astype(F32), gains.shape[1:])
    greet(kv, tp, n_kv, n_tp)
    x_copies = tp_gather(xs, tp, n_tp, x_sem)
    g_copies = tp_gather(gains, tp, n_tp, g_sem)
    for copy in x_copies + g_copies:
        copy.wait_recv()
    stream = [xs[t].astype(F32) for t in range(n_tp)]
    normed = jnp.concatenate(
        [(stream[t] * gains[t][:1]).astype(BF16) for t in range(n_tp)], axis=1
    )
    squares = sum(jnp.sum(s * s, axis=1, keepdims=True) for s in stream)
    sq_copies, sq_total = own_square_total(squares, sq_src, sq_dst, kv, n_kv, rows, sq_sem)
    scatter = PairScatter(kv, n_kv, rows, part, got, summed, got2, sem_a, sem_b)
    for p in range(len(pieces)):
        loads[p].wait()
        scatter.start(p, jnp.dot(normed, w[p], preferred_element_type=F32))
        if p >= LAG:
            scatter.middle(p - LAG)
    for p in range(max(len(pieces) - LAG, 0), len(pieces)):
        scatter.middle(p)
    scale = lax.rsqrt(sq_total() / dim + EPS)
    for p, (i, j) in enumerate(pieces):
        outs[i][:, j * width : (j + 1) * width] = scatter.finish(p) * scale
    scatter.drain()
    for copy in x_copies + g_copies + sq_copies:
        copy.wait_send()


def retain_kernel(heads, dk, dv, q_ref, k_ref, v_ref, g_ref, rate_ref, old_ref, new_ref, mix_ref):
    s = pl.program_id(0)
    q_row = q_ref[pl.ds(s, 1), :]
    k_row = k_ref[pl.ds(s, 1), :] * dk ** (-0.5)
    v_row = v_ref[pl.ds(s, 1), :]
    g_row = g_ref[pl.ds(s, 1), :]
    lines = [q_row[:, h * dk : (h + 1) * dk] for h in range(heads)]
    lines += [k_row[:, h * dk : (h + 1) * dk] for h in range(heads)]
    if len(lines) % 8:
        lines.append(jnp.zeros((8 - len(lines) % 8, dk), F32))
    columns = jnp.concatenate(lines, axis=0).T
    for h in range(heads):
        value = v_row[:, h * dv : (h + 1) * dv]
        query = columns[:, h : h + 1]
        key = columns[:, heads + h : heads + h + 1]
        new = rate_ref[h] * old_ref[0, h] + key * value
        new_ref[0, h] = new
        out = jnp.sum(query * new, axis=0, keepdims=True)
        out = out * lax.rsqrt(jnp.mean(out * out, axis=1, keepdims=True) + EPS)
        gate = g_row[:, h * dv : (h + 1) * dv]
        mix_ref[pl.ds(s, 1), h * dv : (h + 1) * dv] = jax.nn.silu(gate) * out


def mix_kernel(sizes, mix_ref, x_ref, gain_ref, ow_hbm, up_hbm, down_hbm, out_ref, *refs):
    n_kv, n_tp, rows, width, count, dim = sizes
    (ow, up, down, mixes, gains, ends, got_ends, mids, part, got, summed, got2) = refs[:12]
    (sq_src, sq_dst, hid, w_sem, g_sem, mz_sem, my_sem, e_sem, m_sem, sq_sem) = refs[12:22]
    (sem_a, sem_b, hz_sem, hy_sem, f_sem) = refs[22:]
    kv, tp = lax.axis_index("kv"), lax.axis_index("tp")
    z, y = lax.div(kv, PAIR), lax.rem(kv, PAIR)
    block = x_ref.shape[1]
    ow_load = pltpu.make_async_copy(ow_hbm, ow, w_sem.at[0])
    ow_load.start()
    ups, downs = [], []
    for p in range(count):
        load = pltpu.make_async_copy(
            up_hbm.at[:, pl.ds(p * width, width)], up.at[p], w_sem.at[1 + p]
        )
        load.start()
        ups.append(load)
    for p in range(count):
        load = pltpu.make_async_copy(
            down_hbm.at[pl.ds(p * width, width), :], down.at[p], w_sem.at[1 + count + p]
        )
        load.start()
        downs.append(load)
    mixes[0, z, y] = mix_ref[...].astype(BF16)
    gains[tp] = jnp.broadcast_to(gain_ref[...].astype(F32), gains.shape[1:])
    greet(kv, tp, n_kv, n_tp)
    mix_gather = PairGather(kv, n_kv, mixes, mz_sem, my_sem)
    mix_gather.start(0)
    g_copies = tp_gather(gains, tp, n_tp, g_sem)
    mix_gather.relay(0)
    mixed = mix_gather.finish(0)
    ow_load.wait()

    def tp_sum(terms, at, sems):
        for t in range(n_tp):
            ends[at, t] = terms[:, t * block : (t + 1) * block].astype(BF16)
        copies = tp_scatter(ends.at[at], got_ends.at[at], tp, n_tp, sems)
        total = ends[at, tp].astype(F32)
        for d, copy in enumerate(copies):
            copy.wait_recv()
            total = total + got_ends[at, d].astype(F32)
        return copies, total

    e_copies, attention = tp_sum(jnp.dot(mixed, ow[...], preferred_element_type=F32), 0, e_sem)
    mids[tp] = (x_ref[...].astype(F32) + attention).astype(BF16)
    m_copies = tp_gather(mids, tp, n_tp, m_sem)
    for copy in g_copies + m_copies:
        copy.wait_recv()
    stream = [mids[t].astype(F32) for t in range(n_tp)]
    normed = jnp.concatenate(
        [(stream[t] * gains[t][:1]).astype(BF16) for t in range(n_tp)], axis=1
    )
    squares = sum(jnp.sum(s * s, axis=1, keepdims=True) for s in stream)
    sq_copies, sq_total = own_square_total(squares, sq_src, sq_dst, kv, n_kv, rows, sq_sem)
    scatter = PairScatter(kv, n_kv, rows, part, got, summed, got2, sem_a, sem_b)
    gather = PairGather(kv, n_kv, hid, hz_sem, hy_sem)
    for p in range(count):
        ups[p].wait()
        scatter.start(p, jnp.dot(normed, up[p], preferred_element_type=F32))
        if p >= LAG:
            scatter.middle(p - LAG)
    for p in range(max(count - LAG, 0), count):
        scatter.middle(p)
    scale = lax.rsqrt(sq_total() / dim + EPS)
    for p in range(count):
        lifted = scatter.finish(p) * scale
        hid[p, z, y] = jnp.square(jnp.maximum(lifted, 0.0)).astype(BF16)
        gather.start(p)
        if p >= 1:
            gather.relay(p - 1)
    gather.relay(count - 1)
    terms = None
    for p in range(count):
        hidden = gather.finish(p)
        downs[p].wait()
        term = jnp.dot(hidden, down[p], preferred_element_type=F32)
        terms = term if terms is None else terms + term
    f_copies, lowered = tp_sum(terms, 1, f_sem)
    out_ref[...] = (mids[tp].astype(F32) + lowered).astype(BF16)
    mix_gather.drain()
    gather.drain()
    scatter.drain()
    for copy in g_copies + e_copies + m_copies + sq_copies + f_copies:
        copy.wait_send()


VM = pl.BlockSpec(memory_space=pltpu.VMEM)
ANY = pl.BlockSpec(memory_space=pl.ANY)


def scatter_scratch(count, n_kv, rows, width):
    n_z = n_kv // PAIR
    return [
        pltpu.VMEM((count, PAIR, n_z, rows, width), BF16),
        pltpu.VMEM((count, n_z, rows, width), BF16),
        pltpu.VMEM((count, n_z, rows, width), BF16),
        pltpu.VMEM((count, n_z - 1, rows, width), BF16),
    ]


def fused_device(n_kv, n_tp, x, mg, cg, qw, kw, vw, gw, ow, uw, dw, state):
    seqs, heads, dk, dv = state.shape
    batch, block = x.shape
    dim = block * n_kv * n_tp
    n_z = n_kv // PAIR
    depth, width = qw.shape
    counts = tuple(m.shape[1] // width for m in (qw, kw, vw, gw))
    pieces = sum(counts)
    params = functools.partial(
        pltpu.CompilerParams, has_side_effects=True, vmem_limit_bytes=60 * 2**20
    )
    query, key, value, gate = pl.pallas_call(
        functools.partial(project_kernel, (n_kv, n_tp, seqs, width, counts, dim)),
        out_shape=[jax.ShapeDtypeStruct((seqs, m.shape[1]), F32) for m in (qw, kw, vw, gw)],
        in_specs=[VM, VM] + [ANY] * 4,
        out_specs=[VM] * 4,
        scratch_shapes=[
            pltpu.VMEM((n_tp, batch, block), BF16),
            pltpu.VMEM((n_tp, 8, block), F32),
            pltpu.VMEM((pieces, depth, width), BF16),
            *scatter_scratch(pieces, n_kv, seqs, width),
            pltpu.VMEM((n_kv, seqs, 128), F32),
            pltpu.VMEM((n_kv - 1, seqs, 128), F32),
            DMA((pieces,)),
            DMA((2, n_tp - 1)),
            DMA((2, n_tp - 1)),
            DMA((2, n_kv - 1)),
            DMA((2, pieces)),
            DMA((2, pieces, n_z - 1)),
        ],
        compiler_params=params(collective_id=0),
        name="project",
    )(x, mg.reshape(1, block), qw, kw, vw, gw)
    rates = lax.dynamic_slice_in_dim(
        head_decays(HEADS), lax.axis_index("tp") * heads, heads, 0
    )
    whole = lambda a: pl.BlockSpec(a.shape, lambda s: (0, 0))
    state_spec = pl.BlockSpec((1, heads, dk, dv), lambda s: (s, 0, 0, 0))
    new_state, mixed = pl.pallas_call(
        functools.partial(retain_kernel, heads, dk, dv),
        grid=(seqs,),
        out_shape=[
            jax.ShapeDtypeStruct(state.shape, F32),
            jax.ShapeDtypeStruct((seqs, heads * dv), F32),
        ],
        in_specs=[
            whole(query),
            whole(key),
            whole(value),
            whole(gate),
            pl.BlockSpec(memory_space=pltpu.SMEM),
            state_spec,
        ],
        out_specs=[state_spec, pl.BlockSpec((seqs, heads * dv), lambda s: (0, 0))],
        compiler_params=pltpu.CompilerParams(vmem_limit_bytes=32 * 2**20),
        name="retain",
    )(query, key, value, gate, rates, state)
    width = min(1024, uw.shape[1])
    count = uw.shape[1] // width
    out = pl.pallas_call(
        functools.partial(mix_kernel, (n_kv, n_tp, seqs, width, count, dim)),
        out_shape=jax.ShapeDtypeStruct((batch, block), BF16),
        in_specs=[VM, VM, VM, ANY, ANY, ANY],
        out_specs=VM,
        scratch_shapes=[
            pltpu.VMEM(ow.shape, BF16),
            pltpu.VMEM((count, depth, width), BF16),
            pltpu.VMEM((count, width, dw.shape[1]), BF16),
            pltpu.VMEM((1, n_z, PAIR, seqs, heads * dv), BF16),
            pltpu.VMEM((n_tp, 8, block), F32),
            pltpu.VMEM((2, n_tp, batch, block), BF16),
            pltpu.VMEM((2, n_tp - 1, batch, block), BF16),
            pltpu.VMEM((n_tp, batch, block), BF16),
            *scatter_scratch(count, n_kv, seqs, width),
            pltpu.VMEM((n_kv, seqs, 128), F32),
            pltpu.VMEM((n_kv - 1, seqs, 128), F32),
            pltpu.VMEM((count, n_z, PAIR, seqs, width), BF16),
            DMA((1 + 2 * count,)),
            DMA((2, n_tp - 1)),
            DMA((2, 1, n_z - 1)),
            DMA((2, 1, n_z)),
            DMA((2, n_tp - 1)),
            DMA((2, n_tp - 1)),
            DMA((2, n_kv - 1)),
            DMA((2, count)),
            DMA((2, count, n_z - 1)),
            DMA((2, count, n_z - 1)),
            DMA((2, count, n_z)),
            DMA((2, n_tp - 1)),
        ],
        compiler_params=params(collective_id=1),
        name="mix",
    )(mixed, x, cg.reshape(1, block), ow, uw, dw)
    return out, new_state


def solution(mesh):
    return jax.shard_map(
        functools.partial(fused_device, mesh.shape["kv"], mesh.shape["tp"]),
        mesh=mesh,
        in_specs=(
            P(None, ("kv", "tp")),
            P(("kv", "tp")),
            P(("kv", "tp")),
            P("kv", "tp"),
            P("kv", "tp"),
            P("kv", "tp"),
            P("kv", "tp"),
            P("tp", "kv"),
            P("kv", "tp"),
            P("tp", "kv"),
            P("kv", "tp", None, None),
        ),
        out_specs=(P(None, ("kv", "tp")), P("kv", "tp", None, None)),
        check_vma=False,
    )
```
